256 devices in a mesh: fs: 32 (over z, x), rep: 4 (over y), tp: 2 (over core).
Axes of the slice: x: 4, y: 4, z: 8, core: 2. Of those that a mesh axis runs over, the one named last changes fastest.
Arguments:
- inputs: bfloat16 [16384, 2048], P(('fs', 'rep')), may hold values from -24 to 24
- query_cot: bfloat16 [16384, 1024], P(('fs', 'rep'), 'tp'), may hold values from -0.046875 to 0.046875
- attended: bfloat16 [16384, 1024], P(('fs', 'rep')), may hold values from -24 to 24
- output_cot: bfloat16 [16384, 2048], P(('fs', 'rep'), 'tp'), may hold values from -0.046875 to 0.046875
- proj_query: bfloat16 [2048, 256], P('fs'), may hold values from -0.125 to 0.125
- proj_output: bfloat16 [1024, 256], P('fs'), may hold values from -0.1875 to 0.1875
- weight_query: float32 [2048, 1024], P('fs', 'tp'), may hold values from -0.125 to 0.125
- weight_output: float32 [1024, 2048], P('fs', 'tp'), may hold values from -0.1875 to 0.1875
- first_query: float32 [256, 1024], P('fs', 'tp'), may hold values from -6 to 6
- second_query: float32 [256, 1024], P('fs', 'tp'), may hold values from 0.0002 to 2
- first_output: float32 [256, 2048], P('fs', 'tp'), may hold values from -6 to 6
- second_output: float32 [256, 2048], P('fs', 'tp'), may hold values from 0.0002 to 2
Outputs:
- new_weight_query: float32 [2048, 1024], P('fs', 'tp')
- new_weight_output: float32 [1024, 2048], P('fs', 'tp')
- step_query: float32 [2048, 1024], P('fs', 'tp')
- step_output: float32 [1024, 2048], P('fs', 'tp')
- new_first_query: float32 [256, 1024], P('fs', 'tp')
- new_second_query: float32 [256, 1024], P('fs', 'tp')
- new_first_output: float32 [256, 2048], P('fs', 'tp')
- new_second_output: float32 [256, 2048], P('fs', 'tp')
- copy_query: bfloat16 [2048, 1024], P(None, 'tp')
- copy_output: bfloat16 [1024, 2048], P(None, 'tp')
The draws below stay inside these ranges and needn't reach their ends.
All inputs are finite; a program needn't handle non-finite values.
Results may differ from the reference program's by a relative error of at most 0.0031.
Values may be sent and summed in bfloat16 or wider, within the bound.
No kernel may reach another device: no remote copies, remote signals or barrier semaphores. Data moves between devices by JAX's collectives and lax.ppermute only.
A program may use at most 64 MiB of HBM per device.

```python
import jax
import jax.numpy as jnp
from jax import lax

D = 2048
DA = 1024
RANK = 256
TOKENS = 16384


def variance_table(key, height, breadth):
    base = jnp.exp(jax.random.uniform(key, (height, breadth), jnp.float32, jnp.log(0.02), jnp.log(1.0)))
    row_place = jnp.arange(height, dtype=jnp.float32) / height
    col_place = jnp.arange(breadth, dtype=jnp.float32) / breadth
    return base * jnp.exp(-jnp.log(10.0) * row_place)[:, None] * jnp.exp(-jnp.log(10.0) * col_place)[None, :]


def draw_second_query(key, part):
    return variance_table(jax.random.fold_in(key, 11), RANK, DA)


def draw_second_output(key, part):
    return variance_table(jax.random.fold_in(key, 12), RANK, D)


def with_spikes(drawn, stream_key, source, target, parts, factor):
    owner, partner = [(jnp.arange(drawn.shape[axis_at]) // (drawn.shape[axis_at] // parts)).reshape([-1 if axis == axis_at else 1 for axis in range(drawn.ndim)]) for axis_at in (source, target)]
    chosen = jax.random.permutation(stream_key, parts)[partner]
    strong = (owner == chosen) | (owner == (partner + parts // 2) % parts)
    return jnp.where(strong, factor * drawn, drawn)


def block_scale(own_key, extent, cuts, least, top_value):
    factor_of = 1.0
    for axis_at, shards_of in cuts:
        draws = jax.random.uniform(jax.random.fold_in(jax.random.fold_in(own_key, 6), axis_at), (shards_of,), jnp.float32, least / len(cuts), top_value / len(cuts))
        factor_of = factor_of * jnp.repeat(jnp.exp(draws), extent[axis_at] // shards_of).reshape((-1,) + (1,) * (len(extent) - 1 - axis_at))
    return factor_of


def scatter_about(rng, extent, scale, most, pieces=(), kind=jnp.bfloat16):
    values = scale * jax.random.normal(rng, extent, jnp.float32)
    if pieces:
        values = values * block_scale(rng, extent, pieces, -0.22, 0.18)
    return jnp.clip(values, -most, most).astype(kind)


def bell_draw_with(key, shape, scale, reach, pieces, heavy, kind=jnp.bfloat16):
    values = scale * jax.random.normal(key, shape, jnp.float32)
    if pieces:
        values = values * block_scale(key, shape, pieces, -0.22, 0.18)
    return jnp.clip(with_spikes(values, jax.random.fold_in(key, 3), *heavy), -reach, reach).astype(kind)


def setup_inputs(seed: int = 0) -> dict:
    keys = jax.random.split(jax.random.key(seed), 13)
    inputs = bell_draw_with(keys[0], (TOKENS, D), 1.0, 24.0, ((0, 128),), (0, 1, 128, 5.5))
    query_cot = scatter_about(keys[1], (TOKENS, DA), TOKENS ** -0.5, 0.046875, ((0, 128), (1, 2)))
    attended = bell_draw_with(keys[2], (TOKENS, DA), 1.0, 24.0, ((0, 128),), (0, 1, 128, 5.5))
    output_cot = scatter_about(keys[3], (TOKENS, D), TOKENS ** -0.5, 0.046875, ((0, 128), (1, 2)))
    proj_query = scatter_about(keys[4], (D, RANK), D ** -0.5, 0.125, ((0, 32),))
    proj_output = scatter_about(keys[5], (DA, RANK), DA ** -0.5, 0.1875, ((0, 32),))
    weight_query = scatter_about(keys[6], (D, DA), D ** -0.5, 0.125, ((0, 32), (1, 2)), jnp.float32)
    weight_output = scatter_about(keys[7], (DA, D), DA ** -0.5, 0.1875, ((0, 32), (1, 2)), jnp.float32)
    first_query = scatter_about(keys[8], (RANK, DA), 1.0, 6.0, ((0, 32), (1, 2)), jnp.float32)
    second_query = draw_second_query(jax.random.fold_in(keys[12], 71), 0)
    first_output = scatter_about(keys[10], (RANK, D), 1.0, 6.0, ((0, 32), (1, 2)), jnp.float32)
    second_output = draw_second_output(jax.random.fold_in(keys[12], 71), 0)
    return dict(inputs=inputs, query_cot=query_cot, attended=attended, output_cot=output_cot, proj_query=proj_query, proj_output=proj_output, weight_query=weight_query, weight_output=weight_output, first_query=first_query, second_query=second_query, first_output=first_output, second_output=second_output)


beta_first = 0.9
beta_second = 0.95
adam_eps = 1e-08
mean_eps = 1e-06
learn_rate = 0.02

def contract_rows(left, right, high):
    if high:
        return lax.dot_general(left, right, (((0,), (0,)), ((), ())), precision=lax.Precision.HIGHEST, preferred_element_type=jnp.float32)
    return lax.dot_general(left, right, (((0,), (0,)), ((), ())), preferred_element_type=jnp.float32)

def moment_update(low_sum, first, second):
    first_new = beta_first * first + (1.0 - beta_first) * low_sum
    second_new = beta_second * second + (1.0 - beta_second) * low_sum * low_sum
    normed = first_new / (jnp.sqrt(second_new) + adam_eps)
    return (first_new, second_new, normed)

def reference(inputs, query_cot, attended, output_cot, proj_query, proj_output, weight_query, weight_output, first_query, second_query, first_output, second_output):
    grad_query = contract_rows(inputs, query_cot, False)
    grad_output = contract_rows(attended, output_cot, False)
    low_query = contract_rows(proj_query.astype(jnp.float32), grad_query, True)
    low_output = contract_rows(proj_output.astype(jnp.float32), grad_output, True)
    first_q, second_q, normed_q = moment_update(low_query, first_query, second_query)
    first_o, second_o, normed_o = moment_update(low_output, first_output, second_output)
    entries = RANK * (DA + D)
    total = jnp.sum(normed_q * normed_q) + jnp.sum(normed_o * normed_o)
    scale = lax.rsqrt(total / entries + mean_eps)
    half_q = normed_q.astype(jnp.bfloat16)
    half_o = normed_o.astype(jnp.bfloat16)
    step_q = scale * jnp.dot(proj_query, half_q, preferred_element_type=jnp.float32)
    step_o = scale * jnp.dot(proj_output, half_o, preferred_element_type=jnp.float32)
    new_q = weight_query - learn_rate * step_q
    new_o = weight_output - learn_rate * step_o
    return (new_q, new_o, step_q, step_o, first_q, second_q, first_o, second_o, new_q.astype(jnp.bfloat16), new_o.astype(jnp.bfloat16))
```

```python
import jax
import jax.numpy as jnp
from jax import lax
from jax.experimental import pallas as pl
from jax.experimental.pallas import tpu as pltpu
from jax.sharding import Mesh, PartitionSpec as P

D = 2048
DA = 1024
RANK = 256
NZ, NX, NREP, NTP = 8, 4, 4, 2
FS = NZ * NX

beta_first = 0.9
beta_second = 0.95
adam_eps = 1e-08
mean_eps = 1e-06
learn_rate = 0.02

bf16 = jnp.bfloat16
f32 = jnp.float32


def exchange(pieces, axes):
    return lax.all_to_all(pieces, axes, split_axis=0, concat_axis=0, tiled=True)


def from_everyone(shard, axes, devices):
    return exchange(jnp.broadcast_to(shard, (devices, *shard.shape)), axes)


def shifted(array, axis, by):
    n = lax.axis_size(axis)
    return lax.ppermute(array, axis, [(i, (i + by) % n) for i in range(n)])


def one_hot(rows_of, columns, rows):
    r = lax.broadcasted_iota(jnp.int32, (rows, columns), 0)
    return (r == rows_of).astype(bf16)


def rank_of(core):
    k = lax.broadcasted_iota(jnp.int32, (1, RANK // NTP), 1)
    x, j, z = k // 32, (k // 8) % 4, k % 8
    return 8 * (4 * z + x) + 2 * j + core


def finish_kernel(scale_ref, w_ref, p_ref, half_ref, copy_q_ref, copy_o_ref):
    rate = learn_rate
    scale = scale_ref[0, 0]
    p = p_ref[...]
    n = p.shape[0]
    pq = p[:, :64, :].reshape(n * 64, RANK)
    po = p[:, 64:, :].reshape(n * 32, RANK)
    uq = jnp.dot(pq, half_ref[:, :512], preferred_element_type=f32)
    uo = jnp.dot(po, half_ref[:, 512:], preferred_element_type=f32)
    wq = w_ref[:, :64, :].reshape(n * 64, 512)
    copy_q_ref[...] = (wq - rate * (scale * uq)).astype(bf16)
    w0 = w_ref[:, 64:96, :].reshape(n * 32, 512)
    w1 = w_ref[:, 96:, :].reshape(n * 32, 512)
    copy_o_ref[:, :512] = (w0 - rate * (scale * uo[:, :512])).astype(bf16)
    copy_o_ref[:, 512:] = (w1 - rate * (scale * uo[:, 512:])).astype(bf16)


def finish(scale, weights, factors, half):
    step = 4
    return pl.pallas_call(
        finish_kernel,
        grid=(FS // step,),
        in_specs=[
            pl.BlockSpec(memory_space=pltpu.SMEM),
            pl.BlockSpec((step, 128, 512), lambda i: (i, 0, 0)),
            pl.BlockSpec((step, 96, RANK), lambda i: (i, 0, 0)),
            pl.BlockSpec((RANK, 1536), lambda i: (0, 0)),
        ],
        out_specs=[
            pl.BlockSpec((step * 64, 512), lambda i: (i, 0)),
            pl.BlockSpec((step * 32, 1024), lambda i: (i, 0)),
        ],
        out_shape=[
            jax.ShapeDtypeStruct((D, 512), bf16),
            jax.ShapeDtypeStruct((DA, 1024), bf16),
        ],
        name="finish",
    )(scale, weights, factors, half)


def local(
    inputs,
    query_cot,
    attended,
    output_cot,
    proj_query,
    proj_output,
    weight_query,
    weight_output,
    first_query,
    second_query,
    first_output,
    second_output,
):
    z, x = lax.axis_index("z"), lax.axis_index("x")
    rep, core = lax.axis_index("rep"), lax.axis_index("tp")
    fs = z * NX + x

    weights = jnp.concatenate(
        [weight_query, weight_output[:, :512], weight_output[:, 512:]], axis=0
    )
    weights = lax.all_gather(weights, ("z", "x"), axis=0, tiled=True)

    cots = jnp.concatenate([query_cot, output_cot], axis=1)
    cots = [cots, shifted(cots, "rep", 1), shifted(cots, "rep", 2), shifted(cots, "rep", 3)]

    both = jnp.concatenate([proj_query, proj_output], axis=0)
    mine = jnp.dot(both, one_hot(rank_of(core), 128, RANK), preferred_element_type=f32)
    mine = mine.astype(bf16).reshape(NREP, 24, 128)
    piece = lax.dynamic_index_in_dim(mine, rep, 0, keepdims=False)
    piece = from_everyone(piece, "z", NZ)
    piece = from_everyone(piece.reshape(NZ * 24, 128), ("x", "rep"), 16)
    factors = piece.reshape(NX, NREP, NZ, 24, 128).transpose(2, 0, 1, 3, 4)
    factors = factors.reshape(FS, 96, 128)
    factors_q = factors[:, :64].reshape(D, 128)
    factors_o = factors[:, 64:].reshape(DA, 128)

    turned = (((0,), (1,)), ((), ()))
    red_q = lax.dot_general(factors_q, inputs, turned, preferred_element_type=f32)
    red_o = lax.dot_general(factors_o, attended, turned, preferred_element_type=f32)
    red = jnp.stack([red_q, red_o]).reshape(2, NX, NREP, NZ, 128)
    red = red.transpose(2, 0, 1, 3, 4).reshape(NREP, 1, 2, 32, 128)
    red = jnp.broadcast_to(red, (NREP, NTP, 2, 32, 128)).reshape(8, 2, 32, 128)
    red = exchange(red, ("rep", "tp")).reshape(NREP, NTP, 2, 32, 128)

    parts = [
        lax.dynamic_index_in_dim(red, (rep - k) % NREP, 0, keepdims=False)
        for k in range(NREP)
    ]
    left_q = jnp.concatenate([p[:, 0].reshape(64, 128) for p in parts], axis=1)
    left_o = jnp.concatenate([p[:, 1].reshape(64, 128) for p in parts], axis=1)
    right = jnp.concatenate(cots, axis=0).astype(f32)
    part_q = jnp.dot(left_q, right[:, :512], precision=lax.Precision.HIGHEST, preferred_element_type=f32)
    part_o = jnp.dot(left_o, right[:, 512:], precision=lax.Precision.HIGHEST, preferred_element_type=f32)
    part = jnp.concatenate([part_q, part_o], axis=1).reshape(NTP, FS, 1536)
    part = exchange(part.transpose(1, 0, 2), ("x", "z"))
    low = part.sum(axis=0)

    low_rows = [low, shifted(low, "rep", 1), shifted(low, "rep", 2), shifted(low, "rep", 3)]

    def own(a):
        return lax.dynamic_slice_in_dim(a, 2 * rep, 2, 0)

    def moments(low_sum, first, second):
        first_new = beta_first * first + (1.0 - beta_first) * low_sum
        second_new = beta_second * second + (1.0 - beta_second) * low_sum * low_sum
        return first_new, second_new

    def normed_of(low_sum, first, second):
        first_new, second_new = moments(low_sum, first, second)
        return first_new / (jnp.sqrt(second_new) + adam_eps)

    normed_q = normed_of(low[:, :512], own(first_query), own(second_query))
    normed_o = normed_of(low[:, 512:], own(first_output), own(second_output))
    local_total = jnp.sum(normed_q * normed_q) + jnp.sum(normed_o * normed_o)

    def thirds(total):
        high = lax.reduce_precision(total, 8, 7)
        middle = lax.reduce_precision(total - high, 8, 7)
        last = total - high - middle
        lane = lax.broadcasted_iota(jnp.int32, (1, 128), 1)
        row = jnp.where(lane == 0, high, jnp.where(lane == 1, middle, jnp.where(lane == 2, last, 0.0)))
        return row.astype(bf16)

    half = jnp.concatenate([normed_q, normed_o], axis=1).astype(bf16)
    sums = jnp.concatenate([thirds(local_total), jnp.zeros((1, 128), bf16)], axis=0)
    half = from_everyone(jnp.concatenate([half, sums], axis=1), "z", NZ)
    half = from_everyone(half.reshape(16, 1664), ("x", "rep"), 16).reshape(RANK, 1664)
    total = jnp.sum(half[:, 1536:].astype(f32))
    total = total + shifted(total.reshape(1, 1), "tp", 1)[0, 0]
    scale = lax.rsqrt(total / (RANK * (DA + D)) + mean_eps)

    others = shifted(factors, "tp", 1)
    k = lax.broadcasted_iota(jnp.int32, (128, RANK), 0)
    c = lax.broadcasted_iota(jnp.int32, (128, RANK), 1)
    spread = (c == 2 * k + core).astype(bf16)
    spread_other = (c == 2 * k + 1 - core).astype(bf16)
    whole = jnp.dot(factors.reshape(FS * 96, 128), spread, preferred_element_type=f32)
    whole = whole + jnp.dot(others.reshape(FS * 96, 128), spread_other, preferred_element_type=f32)
    whole = whole.astype(bf16).reshape(FS, 96, RANK)
    half = half[:, :1536]

    rows = lax.dynamic_index_in_dim(whole, fs, 0, keepdims=False)
    step_q = scale * jnp.dot(rows[:64], half[:, :512], preferred_element_type=f32)
    step_o = scale * jnp.dot(rows[64:], half[:, 512:], preferred_element_type=f32)
    new_q = weight_query - learn_rate * step_q
    new_o = weight_output - learn_rate * step_o
    copy_q, copy_o = finish(
        scale.reshape(1, 1), weights.reshape(FS, 128, 512), whole, half
    )

    rolled = jnp.stack(low_rows)
    order = (rep - jnp.arange(NREP)) % NREP
    low_all = jnp.take(rolled, order, axis=0).reshape(8, 1536)
    first_q, second_q = moments(low_all[:, :512], first_query, second_query)
    first_o, second_o = moments(low_all[:, 512:], first_output, second_output)
    return (new_q, new_o, step_q, step_o, first_q, second_q, first_o, second_o, copy_q, copy_o)


def solution(mesh):
    devices = mesh.devices.reshape(NZ, NX, NREP, NTP)
    grid = Mesh(devices, ("z", "x", "rep", "tp"))
    fs = ("z", "x")
    tokens = ("z", "x", "rep")
    return jax.shard_map(
        local,
        mesh=grid,
        in_specs=(
            P(tokens, None),
            P(tokens, "tp"),
            P(tokens, None),
            P(tokens, "tp"),
            P(fs, None),
            P(fs, None),
            P(fs, "tp"),
            P(fs, "tp"),
            P(fs, "tp"),
            P(fs, "tp"),
            P(fs, "tp"),
            P(fs, "tp"),
        ),
        out_specs=(
            P(fs, "tp"),
            P(fs, "tp"),
            P(fs, "tp"),
            P(fs, "tp"),
            P(fs, "tp"),
            P(fs, "tp"),
            P(fs, "tp"),
            P(fs, "tp"),
            P(None, "tp"),
            P(None, "tp"),
        ),
        check_vma=False,
    )
```

```python
import jax
import jax.numpy as jnp
from jax import lax
from jax.experimental import pallas as pl
from jax.experimental.pallas import tpu as pltpu
from jax.sharding import Mesh, PartitionSpec as P

D = 2048
DA = 1024
RANK = 256
NZ, NX, NREP, NTP = 8, 4, 4, 2
FS = NZ * NX

beta_first = 0.9
beta_second = 0.95
adam_eps = 1e-08
mean_eps = 1e-06
learn_rate = 0.02

bf16 = jnp.bfloat16
f32 = jnp.float32


def exchange(pieces, axes):
    return lax.all_to_all(pieces, axes, split_axis=0, concat_axis=0, tiled=True)


def from_everyone(shard, axes, devices):
    return exchange(jnp.broadcast_to(shard, (devices, *shard.shape)), axes)


def shifted(array, axis, by):
    n = lax.axis_size(axis)
    return lax.ppermute(array, axis, [(i, (i + by) % n) for i in range(n)])


def one_hot(rows_of, columns, rows):
    r = lax.broadcasted_iota(jnp.int32, (rows, columns), 0)
    return (r == rows_of).astype(bf16)


def rank_of(core):
    k = lax.broadcasted_iota(jnp.int32, (1, RANK // NTP), 1)
    x, j, z = k // 32, (k // 8) % 4, k % 8
    return 8 * (4 * z + x) + 2 * j + core


VMEM = pl.BlockSpec(memory_space=pltpu.VMEM)
SMEM = pl.BlockSpec(memory_space=pltpu.SMEM)


def join_kernel(query_ref, output_ref, both_ref):
    both_ref[:64] = query_ref[...]
    both_ref[64:96] = output_ref[:, :512]
    both_ref[96:] = output_ref[:, 512:]


def join(query, output):
    return pl.pallas_call(
        join_kernel,
        in_specs=[VMEM, VMEM],
        out_specs=VMEM,
        out_shape=jax.ShapeDtypeStruct((128, 512), f32),
        name="join",
    )(query, output)


def project_kernel(factor_ref, inputs_ref, attended_ref, out_ref):
    factors_q = factor_ref[:, :64, :].reshape(D, 128)
    factors_o = factor_ref[:, 64:, :].reshape(DA, 128)
    for n, (left, right) in enumerate(((inputs_ref, factors_q), (attended_ref, factors_o))):
        red = jnp.dot(left[...], right, preferred_element_type=f32).T
        red = red.reshape(NX, NREP, NZ, 128)
        for j in range(NREP):
            mine = red[:, j].reshape(FS, 128)
            out_ref[j, 0, n] = mine
            out_ref[j, 1, n] = mine


def project(factors, inputs, attended):
    return pl.pallas_call(
        project_kernel,
        in_specs=[VMEM, VMEM, VMEM],
        out_specs=VMEM,
        out_shape=jax.ShapeDtypeStruct((NREP, NTP, 2, FS, 128), f32),
        name="project",
    )(factors, inputs, attended)


def partial_kernel(rep_ref, red_ref, c0_ref, c1_ref, c2_ref, c3_ref, out_ref):
    rep = rep_ref[0]
    totals = [None, None]
    for k, cot_ref in enumerate((c0_ref, c1_ref, c2_ref, c3_ref)):
        red = red_ref[lax.rem(rep + (NREP - k), NREP)]
        for n, (low, high) in enumerate(((0, 512), (512, 1536))):
            left = red[:, n].reshape(64, 128)
            first = left.astype(bf16)
            rest = left - first.astype(f32)
            second = rest.astype(bf16)
            third = (rest - second.astype(f32)).astype(bf16)
            terms = jnp.concatenate([first, second, third], axis=0)
            part = jnp.dot(terms, cot_ref[:, low:high], preferred_element_type=f32)
            totals[n] = part if totals[n] is None else totals[n] + part
    for n, (low, high) in enumerate(((0, 512), (512, 1536))):
        part = totals[n]
        part = part[:64] + (part[64:128] + part[128:])
        out_ref[:, 0, low:high] = part[:32]
        out_ref[:, 1, low:high] = part[32:]


def partial_sums(rep, red, cots):
    return pl.pallas_call(
        partial_kernel,
        in_specs=[SMEM] + [VMEM] * 5,
        out_specs=VMEM,
        out_shape=jax.ShapeDtypeStruct((FS, NTP, 1536), f32),
        name="partial_sums",
    )(rep, red, *cots)


def moments(low_sum, first, second):
    first_new = beta_first * first + (1.0 - beta_first) * low_sum
    second_new = beta_second * second + (1.0 - beta_second) * low_sum * low_sum
    return first_new, second_new


def own_rows(ref, rep):
    value = ref[...]
    rows = value[:2]
    for k in range(1, NREP):
        rows = jnp.where(rep == k, value[2 * k : 2 * k + 2], rows)
    return rows


def normed_kernel(rep_ref, part_ref, fq_ref, sq_ref, fo_ref, so_ref, low_ref, half_ref):
    rep = rep_ref[0]
    low = part_ref[0]
    for k in range(1, FS):
        low = low + part_ref[k]
    low_ref[...] = low
    pieces = []
    total = jnp.zeros((2, 1), f32)
    for low_sum, first_ref, second_ref in (
        (low[:, :512], fq_ref, sq_ref),
        (low[:, 512:], fo_ref, so_ref),
    ):
        first_new, second_new = moments(low_sum, own_rows(first_ref, rep), own_rows(second_ref, rep))
        normed = first_new / (jnp.sqrt(second_new) + adam_eps)
        total = total + jnp.sum(normed * normed, axis=1, keepdims=True)
        pieces.append(normed.astype(bf16))
    high = total.astype(bf16).astype(f32)
    middle = (total - high).astype(bf16).astype(f32)
    last = total - high - middle
    lane = lax.broadcasted_iota(jnp.int32, (2, 128), 1)
    sums = jnp.where(lane == 0, high, jnp.where(lane == 1, middle, jnp.where(lane == 2, last, 0.0)))
    payload = jnp.concatenate(pieces + [sums.astype(bf16)], axis=1)
    for k in range(NZ):
        half_ref[k] = payload


def normed_payload(rep, part, first_query, second_query, first_output, second_output):
    return pl.pallas_call(
        normed_kernel,
        in_specs=[SMEM] + [VMEM] * 5,
        out_specs=[VMEM, VMEM],
        out_shape=[
            jax.ShapeDtypeStruct((2, 1536), f32),
            jax.ShapeDtypeStruct((NZ, 2, 1664), bf16),
        ],
        name="normed_payload",
    )(rep, part, first_query, second_query, first_output, second_output)


def finish_kernel(
    mine_ref, other_ref, half_ref, rows_ref, wq_ref, wo_ref, w_ref, p_ref,
    copy_q_ref, copy_o_ref, step_q_ref, step_o_ref, new_q_ref, new_o_ref,
):
    total = jnp.full((1, 128), mine_ref[0, 0] + other_ref[0, 0], f32)
    scale = lax.rsqrt(total / (RANK * (DA + D)) + mean_eps)[:, :1]

    @pl.when(pl.program_id(0) == 0)
    def _():
        rows = rows_ref[...]
        uq = jnp.dot(rows[:64], half_ref[:, :512], preferred_element_type=f32)
        uo = jnp.dot(rows[64:], half_ref[:, 512:1536], preferred_element_type=f32)
        step_q = scale * uq
        step_o = scale * uo
        step_q_ref[...] = step_q
        step_o_ref[...] = step_o
        new_q_ref[...] = wq_ref[...] - learn_rate * step_q
        new_o_ref[...] = wo_ref[...] - learn_rate * step_o

    p = p_ref[...]
    n = p.shape[0]
    pq = p[:, :64, :].reshape(n * 64, RANK)
    po = p[:, 64:, :].reshape(n * 32, RANK)
    uq = jnp.dot(pq, half_ref[:, :512], preferred_element_type=f32)
    uo = jnp.dot(po, half_ref[:, 512:1536], preferred_element_type=f32)
    wq = w_ref[:, :64, :].reshape(n * 64, 512)
    copy_q_ref[...] = (wq - learn_rate * (scale * uq)).astype(bf16)
    w0 = w_ref[:, 64:96, :].reshape(n * 32, 512)
    w1 = w_ref[:, 96:, :].reshape(n * 32, 512)
    copy_o_ref[:, :512] = (w0 - learn_rate * (scale * uo[:, :512])).astype(bf16)
    copy_o_ref[:, 512:] = (w1 - learn_rate * (scale * uo[:, 512:])).astype(bf16)


def finish(mine, other, half, rows, weight_query, weight_output, weights, factors):
    step = 4
    def whole(shape):
        return pl.BlockSpec(shape, lambda i: (0,) * len(shape))

    return pl.pallas_call(
        finish_kernel,
        grid=(FS // step,),
        in_specs=[
            SMEM,
            SMEM,
            whole((RANK, 1664)),
            whole((96, RANK)),
            whole((64, 512)),
            whole((32, 1024)),
            pl.BlockSpec((step, 128, 512), lambda i: (i, 0, 0)),
            pl.BlockSpec((step, 96, RANK), lambda i: (i, 0, 0)),
        ],
        out_specs=[
            pl.BlockSpec((step * 64, 512), lambda i: (i, 0)),
            pl.BlockSpec((step * 32, 1024), lambda i: (i, 0)),
            whole((64, 512)),
            whole((32, 1024)),
            whole((64, 512)),
            whole((32, 1024)),
        ],
        out_shape=[
            jax.ShapeDtypeStruct((D, 512), bf16),
            jax.ShapeDtypeStruct((DA, 1024), bf16),
            jax.ShapeDtypeStruct((64, 512), f32),
            jax.ShapeDtypeStruct((32, 1024), f32),
            jax.ShapeDtypeStruct((64, 512), f32),
            jax.ShapeDtypeStruct((32, 1024), f32),
        ],
        name="finish",
    )(mine, other, half, rows, weight_query, weight_output, weights, factors)


def local(
    inputs,
    query_cot,
    attended,
    output_cot,
    proj_query,
    proj_output,
    weight_query,
    weight_output,
    first_query,
    second_query,
    first_output,
    second_output,
):
    z, x = lax.axis_index("z"), lax.axis_index("x")
    rep, core = lax.axis_index("rep"), lax.axis_index("tp")
    fs = z * NX + x

    here = rep.reshape(1)

    weights = join(weight_query, weight_output)
    weights = lax.all_gather(weights, ("z", "x"), axis=0, tiled=True)

    cots = jnp.concatenate([query_cot, output_cot], axis=1)
    cots = [cots, shifted(cots, "rep", 1), shifted(cots, "rep", 2), shifted(cots, "rep", 3)]

    both = jnp.concatenate([proj_query, proj_output], axis=0)
    mine = jnp.dot(both, one_hot(rank_of(core), 128, RANK), preferred_element_type=f32)
    factors = from_everyone(mine.astype(bf16).reshape(96, 128), ("z", "x"), FS)

    red = project(factors, inputs, attended).reshape(8, 2, FS, 128)
    red = exchange(red, ("rep", "tp")).reshape(NREP, NTP, 2, FS, 128)
    part = exchange(partial_sums(here, red, cots), ("x", "z"))
    low, half = normed_payload(
        here, part, first_query, second_query, first_output, second_output
    )
    half = exchange(half, "z")
    low, half = lax.optimization_barrier((low, half))
    low_rows = [low, shifted(low, "rep", 1), shifted(low, "rep", 2), shifted(low, "rep", 3)]
    half = from_everyone(half.reshape(16, 1664), ("x", "rep"), 16).reshape(RANK, 1664)
    total = jnp.sum(half[:, 1536:].astype(f32)).reshape(1, 1)
    other = shifted(total, "tp", 1)

    others = shifted(factors, "tp", 1)
    k = lax.broadcasted_iota(jnp.int32, (128, RANK), 0)
    c = lax.broadcasted_iota(jnp.int32, (128, RANK), 1)
    spread = (c == 2 * k + core).astype(bf16)
    spread_other = (c == 2 * k + 1 - core).astype(bf16)
    whole = jnp.dot(factors.reshape(FS * 96, 128), spread, preferred_element_type=f32)
    whole = whole + jnp.dot(others.reshape(FS * 96, 128), spread_other, preferred_element_type=f32)
    whole = whole.astype(bf16).reshape(FS, 96, RANK)
    rows = lax.dynamic_index_in_dim(whole, fs, 0, keepdims=False)

    copy_q, copy_o, step_q, step_o, new_q, new_o = finish(
        total, other, half, rows, weight_query, weight_output,
        weights.reshape(FS, 128, 512), whole,
    )

    rolled = jnp.stack(low_rows)
    order = (rep - jnp.arange(NREP)) % NREP
    low_all = jnp.take(rolled, order, axis=0).reshape(8, 1536)
    first_q, second_q = moments(low_all[:, :512], first_query, second_query)
    first_o, second_o = moments(low_all[:, 512:], first_output, second_output)
    return (new_q, new_o, step_q, step_o, first_q, second_q, first_o, second_o, copy_q, copy_o)


def solution(mesh):
    devices = mesh.devices.reshape(NZ, NX, NREP, NTP)
    grid = Mesh(devices, ("z", "x", "rep", "tp"))
    fs = ("z", "x")
    tokens = ("z", "x", "rep")
    return jax.shard_map(
        local,
        mesh=grid,
        in_specs=(
            P(tokens, None),
            P(tokens, "tp"),
            P(tokens, None),
            P(tokens, "tp"),
            P(fs, None),
            P(fs, None),
            P(fs, "tp"),
            P(fs, "tp"),
            P(fs, "tp"),
            P(fs, "tp"),
            P(fs, "tp"),
            P(fs, "tp"),
        ),
        out_specs=(
            P(fs, "tp"),
            P(fs, "tp"),
            P(fs, "tp"),
            P(fs, "tp"),
            P(fs, "tp"),
            P(fs, "tp"),
            P(fs, "tp"),
            P(fs, "tp"),
            P(None, "tp"),
            P(None, "tp"),
        ),
        check_vma=False,
    )
```

```python
import jax
import jax.numpy as jnp
from jax import lax
from jax.experimental import pallas as pl
from jax.experimental.pallas import tpu as pltpu
from jax.sharding import Mesh, PartitionSpec as P


D = 2048
DA = 1024
RANK = 256
NZ, NX, NREP, NTP = 8, 4, 4, 2
FS = NZ * NX

beta_first = 0.9
beta_second = 0.95
adam_eps = 1e-08
mean_eps = 1e-06
learn_rate = 0.02

bf16 = jnp.bfloat16
f32 = jnp.float32


def exchange(pieces, axes):
    return lax.all_to_all(pieces, axes, split_axis=0, concat_axis=0, tiled=True)


def from_everyone(shard, axes, devices):
    return exchange(jnp.broadcast_to(shard, (devices, *shard.shape)), axes)


def shifted(array, axis, by):
    n = lax.axis_size(axis)
    return lax.ppermute(array, axis, [(i, (i + by) % n) for i in range(n)])


def one_hot(rows_of, columns, rows):
    r = lax.broadcasted_iota(jnp.int32, (rows, columns), 0)
    return (r == rows_of).astype(bf16)


def rank_of(core):
    k = lax.broadcasted_iota(jnp.int32, (1, RANK // NTP), 1)
    x, j, z = k // 32, (k // 8) % 4, k % 8
    return 8 * (4 * z + x) + 2 * j + core


VMEM = pl.BlockSpec(memory_space=pltpu.VMEM)


def near(array):
    return pltpu.with_memory_space_constraint(array, pltpu.VMEM)


SMEM = pl.BlockSpec(memory_space=pltpu.SMEM)


def join_kernel(query_ref, output_ref, both_ref):
    both_ref[:64] = query_ref[...]
    both_ref[64:96] = output_ref[:, :512]
    both_ref[96:] = output_ref[:, 512:]


def join(query, output):
    return pl.pallas_call(
        join_kernel,
        in_specs=[VMEM, VMEM],
        out_specs=VMEM,
        out_shape=jax.ShapeDtypeStruct((128, 512), f32),
        name="join",
    )(query, output)


def project_kernel(factor_ref, inputs_ref, attended_ref, out_ref):
    factors_q = factor_ref[:, :64, :].reshape(D, 128)
    factors_o = factor_ref[:, 64:, :].reshape(DA, 128)
    for n, (left, right) in enumerate(((inputs_ref, factors_q), (attended_ref, factors_o))):
        red = jnp.dot(left[...], right, preferred_element_type=f32).T
        red = red.reshape(NX, NREP, NZ, 128)
        for j in range(NREP):
            mine = red[:, j].reshape(FS, 128)
            out_ref[j, 0, n] = mine
            out_ref[j, 1, n] = mine


def project(factors, inputs, attended):
    return pl.pallas_call(
        project_kernel,
        in_specs=[VMEM, VMEM, VMEM],
        out_specs=VMEM,
        out_shape=pltpu.VMEM((NREP, NTP, 2, FS, 128), f32),
        name="project",
    )(near(factors), near(inputs), near(attended))


def partial_kernel(rep_ref, red_ref, query_ref, output_ref, c1_ref, c2_ref, c3_ref, out_ref):
    rep = rep_ref[0]
    totals = [None, None]
    own = (query_ref[...], output_ref[...])
    sent = [(c[:, :512], c[:, 512:]) for c in (c1_ref, c2_ref, c3_ref)]
    for k, cots in enumerate([own] + sent):
        red = red_ref[lax.rem(rep + (NREP - k), NREP)]
        for n in range(2):
            left = red[:, n].reshape(64, 128)
            first = left.astype(bf16)
            rest = left - first.astype(f32)
            second = rest.astype(bf16)
            third = (rest - second.astype(f32)).astype(bf16)
            terms = jnp.concatenate([first, second, third], axis=0)
            part = jnp.dot(terms, cots[n], preferred_element_type=f32)
            totals[n] = part if totals[n] is None else totals[n] + part
    for n, (low, high) in enumerate(((0, 512), (512, 1536))):
        part = totals[n]
        part = part[:64] + (part[64:128] + part[128:])
        out_ref[:, 0, low:high] = part[:32]
        out_ref[:, 1, low:high] = part[32:]


def partial_sums(rep, red, cots):
    return pl.pallas_call(
        partial_kernel,
        in_specs=[SMEM] + [VMEM] * 6,
        out_specs=VMEM,
        out_shape=pltpu.VMEM((FS, NTP, 1536), f32),
        name="partial_sums",
    )(rep, near(red), *[near(c) for c in cots])


def moments(low_sum, first, second):
    first_new = beta_first * first + (1.0 - beta_first) * low_sum
    second_new = beta_second * second + (1.0 - beta_second) * low_sum * low_sum
    return first_new, second_new


def own_rows(ref, rep):
    value = ref[...]
    rows = value[:2]
    for k in range(1, NREP):
        rows = jnp.where(rep == k, value[2 * k : 2 * k + 2], rows)
    return rows


def normed_kernel(rep_ref, part_ref, fq_ref, sq_ref, fo_ref, so_ref, low_ref, half_ref):
    rep = rep_ref[0]
    low = part_ref[0]
    for k in range(1, FS):
        low = low + part_ref[k]
    low_ref[...] = low
    pieces = []
    total = jnp.zeros((2, 1), f32)
    for low_sum, first_ref, second_ref in (
        (low[:, :512], fq_ref, sq_ref),
        (low[:, 512:], fo_ref, so_ref),
    ):
        first_new, second_new = moments(low_sum, own_rows(first_ref, rep), own_rows(second_ref, rep))
        normed = first_new / (jnp.sqrt(second_new) + adam_eps)
        total = total + jnp.sum(normed * normed, axis=1, keepdims=True)
        pieces.append(normed.astype(bf16))
    high = total.astype(bf16).astype(f32)
    middle = (total - high).astype(bf16).astype(f32)
    last = total - high - middle
    lane = lax.broadcasted_iota(jnp.int32, (2, 128), 1)
    sums = jnp.where(lane == 0, high, jnp.where(lane == 1, middle, jnp.where(lane == 2, last, 0.0)))
    payload = jnp.concatenate(pieces + [sums.astype(bf16)], axis=1)
    for k in range(NZ):
        half_ref[k] = payload


def normed_payload(rep, part, first_query, second_query, first_output, second_output):
    return pl.pallas_call(
        normed_kernel,
        in_specs=[SMEM] + [VMEM] * 5,
        out_specs=[VMEM, VMEM],
        out_shape=[
            pltpu.VMEM((2, 1536), f32),
            pltpu.VMEM((NZ, 2, 1664), bf16),
        ],
        name="normed_payload",
    )(rep, *[near(a) for a in (part, first_query, second_query, first_output, second_output)])


def finish_kernel(
    mine_ref, other_ref, half_ref, rows_ref, wq_ref, wo_ref, w_ref, p_ref,
    copy_q_ref, copy_o_ref, step_q_ref, step_o_ref, new_q_ref, new_o_ref,
):
    total = jnp.full((1, 128), mine_ref[0, 0] + other_ref[0, 0], f32)
    scale = lax.rsqrt(total / (RANK * (DA + D)) + mean_eps)[:, :1]

    @pl.when(pl.program_id(0) == 0)
    def _():
        rows = rows_ref[...]
        uq = jnp.dot(rows[:64], half_ref[:, :512], preferred_element_type=f32)
        uo = jnp.dot(rows[64:], half_ref[:, 512:1536], preferred_element_type=f32)
        step_q = scale * uq
        step_o = scale * uo
        step_q_ref[...] = step_q
        step_o_ref[...] = step_o
        new_q_ref[...] = wq_ref[...] - learn_rate * step_q
        new_o_ref[...] = wo_ref[...] - learn_rate * step_o

    p = p_ref[...]
    n = p.shape[0]
    pq = p[:, :64, :].reshape(n * 64, RANK)
    po = p[:, 64:, :].reshape(n * 32, RANK)
    uq = jnp.dot(pq, half_ref[:, :512], preferred_element_type=f32)
    uo = jnp.dot(po, half_ref[:, 512:1536], preferred_element_type=f32)
    wq = w_ref[:, :64, :].reshape(n * 64, 512)
    copy_q_ref[...] = (wq - learn_rate * (scale * uq)).astype(bf16)
    w0 = w_ref[:, 64:96, :].reshape(n * 32, 512)
    w1 = w_ref[:, 96:, :].reshape(n * 32, 512)
    copy_o_ref[:, :512] = (w0 - learn_rate * (scale * uo[:, :512])).astype(bf16)
    copy_o_ref[:, 512:] = (w1 - learn_rate * (scale * uo[:, 512:])).astype(bf16)


def finish(mine, other, half, rows, weight_query, weight_output, weights, factors):
    step = 8

    def whole(shape):
        return pl.BlockSpec(shape, lambda i: (0,) * len(shape))

    return pl.pallas_call(
        finish_kernel,
        grid=(FS // step,),
        in_specs=[
            SMEM,
            SMEM,
            whole((RANK, 1664)),
            whole((96, RANK)),
            whole((64, 512)),
            whole((32, 1024)),
            pl.BlockSpec((step, 128, 512), lambda i: (i, 0, 0)),
            pl.BlockSpec((step, 96, RANK), lambda i: (i, 0, 0)),
        ],
        out_specs=[
            pl.BlockSpec((step * 64, 512), lambda i: (i, 0)),
            pl.BlockSpec((step * 32, 1024), lambda i: (i, 0)),
            whole((64, 512)),
            whole((32, 1024)),
            whole((64, 512)),
            whole((32, 1024)),
        ],
        out_shape=[
            jax.ShapeDtypeStruct((D, 512), bf16),
            jax.ShapeDtypeStruct((DA, 1024), bf16),
            jax.ShapeDtypeStruct((64, 512), f32),
            jax.ShapeDtypeStruct((32, 1024), f32),
            jax.ShapeDtypeStruct((64, 512), f32),
            jax.ShapeDtypeStruct((32, 1024), f32),
        ],
        name="finish",
    )(mine, other, half, rows, weight_query, weight_output, weights, factors)


def local(
    inputs,
    query_cot,
    attended,
    output_cot,
    proj_query,
    proj_output,
    weight_query,
    weight_output,
    first_query,
    second_query,
    first_output,
    second_output,
):
    z, x = lax.axis_index("z"), lax.axis_index("x")
    rep, core = lax.axis_index("rep"), lax.axis_index("tp")
    fs = z * NX + x

    here = rep.reshape(1)

    weights = join(weight_query, weight_output)
    weights = lax.all_gather(weights, ("z", "x"), axis=0, tiled=True)

    cots = jnp.concatenate([query_cot, output_cot], axis=1)
    cots = [shifted(cots, "rep", 1), shifted(cots, "rep", 2), shifted(cots, "rep", 3)]

    both = jnp.concatenate([proj_query, proj_output], axis=0)
    mine = jnp.dot(both, one_hot(rank_of(core), 128, RANK), preferred_element_type=f32)
    factors = from_everyone(mine.astype(bf16).reshape(96, 128), ("z", "x"), FS)

    red = project(factors, inputs, attended).reshape(8, 2, FS, 128)
    red = exchange(red, ("rep", "tp")).reshape(NREP, NTP, 2, FS, 128)
    part = exchange(partial_sums(here, red, [query_cot, output_cot] + cots), ("x", "z"))
    low, half = normed_payload(
        here, part, first_query, second_query, first_output, second_output
    )
    half = exchange(half, "z")
    low, half = lax.optimization_barrier((low, half))
    low_rows = [low, shifted(low, "rep", 1), shifted(low, "rep", 2), shifted(low, "rep", 3)]
    half = from_everyone(half.reshape(16, 1664), ("x", "rep"), 16).reshape(RANK, 1664)
    total = jnp.sum(half[:, 1536:].astype(f32)).reshape(1, 1)
    other = shifted(total, "tp", 1)

    others = shifted(factors, "tp", 1)
    k = lax.broadcasted_iota(jnp.int32, (128, RANK), 0)
    c = lax.broadcasted_iota(jnp.int32, (128, RANK), 1)
    spread = (c == 2 * k + core).astype(bf16)
    spread_other = (c == 2 * k + 1 - core).astype(bf16)
    whole = jnp.dot(factors.reshape(FS * 96, 128), spread, preferred_element_type=f32)
    whole = whole + jnp.dot(others.reshape(FS * 96, 128), spread_other, preferred_element_type=f32)
    whole = whole.astype(bf16).reshape(FS, 96, RANK)
    rows = lax.dynamic_index_in_dim(whole, fs, 0, keepdims=False)

    copy_q, copy_o, step_q, step_o, new_q, new_o = finish(
        total, other, half, rows, weight_query, weight_output,
        weights.reshape(FS, 128, 512), whole,
    )

    rolled = jnp.stack(low_rows)
    order = (rep - jnp.arange(NREP)) % NREP
    low_all = jnp.take(rolled, order, axis=0).reshape(8, 1536)
    first_q, second_q = moments(low_all[:, :512], first_query, second_query)
    first_o, second_o = moments(low_all[:, 512:], first_output, second_output)
    return (new_q, new_o, step_q, step_o, first_q, second_q, first_o, second_o, copy_q, copy_o)


def solution(mesh):
    devices = mesh.devices.reshape(NZ, NX, NREP, NTP)
    grid = Mesh(devices, ("z", "x", "rep", "tp"))
    fs = ("z", "x")
    tokens = ("z", "x", "rep")
    return jax.shard_map(
        local,
        mesh=grid,
        in_specs=(
            P(tokens, None),
            P(tokens, "tp"),
            P(tokens, None),
            P(tokens, "tp"),
            P(fs, None),
            P(fs, None),
            P(fs, "tp"),
            P(fs, "tp"),
            P(fs, "tp"),
            P(fs, "tp"),
            P(fs, "tp"),
            P(fs, "tp"),
        ),
        out_specs=(
            P(fs, "tp"),
            P(fs, "tp"),
            P(fs, "tp"),
            P(fs, "tp"),
            P(fs, "tp"),
            P(fs, "tp"),
            P(fs, "tp"),
            P(fs, "tp"),
            P(None, "tp"),
            P(None, "tp"),
        ),
        check_vma=False,
    )
```

```python
import jax
import jax.numpy as jnp
from jax import lax
from jax.experimental import pallas as pl
from jax.experimental.pallas import tpu as pltpu
from jax.sharding import Mesh, PartitionSpec as P


D = 2048
DA = 1024
RANK = 256
NZ, NX, NREP, NTP = 8, 4, 4, 2
FS = NZ * NX

beta_first = 0.9
beta_second = 0.95
adam_eps = 1e-08
mean_eps = 1e-06
learn_rate = 0.02

bf16 = jnp.bfloat16
f32 = jnp.float32


def exchange(pieces, axes):
    return lax.all_to_all(pieces, axes, split_axis=0, concat_axis=0, tiled=True)


def from_everyone(shard, axes, devices):
    return exchange(jnp.broadcast_to(shard, (devices, *shard.shape)), axes)


def shifted(array, axis, by):
    n = lax.axis_size(axis)
    return lax.ppermute(array, axis, [(i, (i + by) % n) for i in range(n)])


VMEM = pl.BlockSpec(memory_space=pltpu.VMEM)


def near(array):
    return pltpu.with_memory_space_constraint(array, pltpu.VMEM)


SMEM = pl.BlockSpec(memory_space=pltpu.SMEM)


def join_kernel(query_ref, output_ref, both_ref):
    both_ref[:64] = query_ref[...]
    both_ref[64:96] = output_ref[:, :512]
    both_ref[96:] = output_ref[:, 512:]


def join(query, output):
    return pl.pallas_call(
        join_kernel,
        in_specs=[VMEM, VMEM],
        out_specs=VMEM,
        out_shape=jax.ShapeDtypeStruct((128, 512), f32),
        name="join",
    )(query, output)


def select_kernel(place_ref, query_ref, output_ref, out_ref):
    rep, core = place_ref[0], place_ref[1]
    both = jnp.concatenate([query_ref[...], output_ref[...]], axis=0)
    i = lax.broadcasted_iota(jnp.int32, (24, 96), 0)
    r = lax.broadcasted_iota(jnp.int32, (24, 96), 1)
    rows = (r == jnp.where(i < 16, 16 * rep + i, 48 + 8 * rep + i)).astype(bf16)
    k = lax.broadcasted_iota(jnp.int32, (RANK, 128), 1)
    r = lax.broadcasted_iota(jnp.int32, (RANK, 128), 0)
    ranks = (r == 32 * (k % 8) + 8 * (k // 32) + 2 * ((k // 8) % 4) + core).astype(bf16)
    chosen = jnp.dot(rows, both, preferred_element_type=f32).astype(bf16)
    chosen = jnp.dot(chosen, ranks, preferred_element_type=f32).astype(bf16)
    for n in range(NZ):
        out_ref[n] = chosen


def select(place, query, output):
    return pl.pallas_call(
        select_kernel,
        in_specs=[SMEM, VMEM, VMEM],
        out_specs=VMEM,
        out_shape=pltpu.VMEM((NZ, 24, 128), bf16),
        name="select",
    )(place, query, output)


def project_kernel(piece_ref, inputs_ref, attended_ref, red_ref, factor_ref):
    for z in range(NZ):
        for x in range(NX):
            for j in range(NREP):
                n, at = NX * z + x, 24 * z
                factor_ref[n, 16 * j : 16 * j + 16] = piece_ref[NREP * x + j, at : at + 16]
                factor_ref[n, 64 + 8 * j : 72 + 8 * j] = piece_ref[NREP * x + j, at + 16 : at + 24]
    factors_q = factor_ref[:, :64, :].reshape(D, 128)
    factors_o = factor_ref[:, 64:, :].reshape(DA, 128)
    for n, (left, right) in enumerate(((inputs_ref, factors_q), (attended_ref, factors_o))):
        red = jnp.dot(left[...], right, preferred_element_type=f32).T
        red = red.reshape(NX, NREP, NZ, 128)
        for j in range(NREP):
            mine = red[:, j].reshape(FS, 128)
            red_ref[j, 0, n] = mine
            red_ref[j, 1, n] = mine


def project(pieces, inputs, attended):
    return pl.pallas_call(
        project_kernel,
        in_specs=[VMEM, VMEM, VMEM],
        out_specs=[VMEM, VMEM],
        out_shape=[
            pltpu.VMEM((NREP, NTP, 2, FS, 128), f32),
            pltpu.VMEM((FS, 96, 128), bf16),
        ],
        name="project",
    )(near(pieces), near(inputs), near(attended))


def partial_kernel(rep_ref, red_ref, query_ref, output_ref, c1_ref, c2_ref, c3_ref, out_ref):
    rep = rep_ref[0]
    totals = [None, None]
    own = (query_ref[...], output_ref[...])
    sent = [(c[:, :512], c[:, 512:]) for c in (c1_ref, c2_ref, c3_ref)]
    for k, cots in enumerate([own] + sent):
        red = red_ref[lax.rem(rep + (NREP - k), NREP)]
        for n in range(2):
            left = red[:, n].reshape(64, 128)
            first = left.astype(bf16)
            rest = left - first.astype(f32)
            second = rest.astype(bf16)
            third = (rest - second.astype(f32)).astype(bf16)
            terms = jnp.concatenate([first, second, third], axis=0)
            part = jnp.dot(terms, cots[n], preferred_element_type=f32)
            totals[n] = part if totals[n] is None else totals[n] + part
    for n, (low, high) in enumerate(((0, 512), (512, 1536))):
        part = totals[n]
        part = part[:64] + (part[64:128] + part[128:])
        out_ref[:, 0, low:high] = part[:32]
        out_ref[:, 1, low:high] = part[32:]


def partial_sums(rep, red, cots):
    return pl.pallas_call(
        partial_kernel,
        in_specs=[SMEM] + [VMEM] * 6,
        out_specs=VMEM,
        out_shape=pltpu.VMEM((FS, NTP, 1536), f32),
        name="partial_sums",
    )(rep, near(red), *[near(c) for c in cots])


def moments(low_sum, first, second):
    first_new = beta_first * first + (1.0 - beta_first) * low_sum
    second_new = beta_second * second + (1.0 - beta_second) * low_sum * low_sum
    return first_new, second_new


def own_rows(ref, rep):
    value = ref[...]
    rows = value[:2]
    for k in range(1, NREP):
        rows = jnp.where(rep == k, value[2 * k : 2 * k + 2], rows)
    return rows


def normed_kernel(rep_ref, part_ref, fq_ref, sq_ref, fo_ref, so_ref, low_ref, half_ref):
    rep = rep_ref[0]
    low = part_ref[0]
    for k in range(1, FS):
        low = low + part_ref[k]
    low_ref[...] = low
    pieces = []
    total = jnp.zeros((2, 1), f32)
    for low_sum, first_ref, second_ref in (
        (low[:, :512], fq_ref, sq_ref),
        (low[:, 512:], fo_ref, so_ref),
    ):
        first_new, second_new = moments(low_sum, own_rows(first_ref, rep), own_rows(second_ref, rep))
        normed = first_new / (jnp.sqrt(second_new) + adam_eps)
        total = total + jnp.sum(normed * normed, axis=1, keepdims=True)
        pieces.append(normed.astype(bf16))
    high = total.astype(bf16).astype(f32)
    middle = (total - high).astype(bf16).astype(f32)
    last = total - high - middle
    lane = lax.broadcasted_iota(jnp.int32, (2, 128), 1)
    sums = jnp.where(lane == 0, high, jnp.where(lane == 1, middle, jnp.where(lane == 2, last, 0.0)))
    payload = jnp.concatenate(pieces + [sums.astype(bf16)], axis=1)
    for k in range(NZ):
        half_ref[k] = payload


def normed_payload(rep, part, first_query, second_query, first_output, second_output):
    return pl.pallas_call(
        normed_kernel,
        in_specs=[SMEM] + [VMEM] * 5,
        out_specs=[VMEM, VMEM],
        out_shape=[
            pltpu.VMEM((2, 1536), f32),
            pltpu.VMEM((NZ, 2, 1664), bf16),
        ],
        name="normed_payload",
    )(rep, *[near(a) for a in (part, first_query, second_query, first_output, second_output)])


def finish_kernel(
    mine_ref, other_ref, half_ref, rows_ref, wq_ref, wo_ref, w_ref, p_ref,
    copy_q_ref, copy_o_ref, step_q_ref, step_o_ref, new_q_ref, new_o_ref,
):
    total = jnp.full((1, 128), mine_ref[0, 0] + other_ref[0, 0], f32)
    scale = lax.rsqrt(total / (RANK * (DA + D)) + mean_eps)[:, :1]

    @pl.when(pl.program_id(0) == 0)
    def _():
        rows = rows_ref[...]
        uq = jnp.dot(rows[:64], half_ref[:, :512], preferred_element_type=f32)
        uo = jnp.dot(rows[64:], half_ref[:, 512:1536], preferred_element_type=f32)
        step_q = scale * uq
        step_o = scale * uo
        step_q_ref[...] = step_q
        step_o_ref[...] = step_o
        new_q_ref[...] = wq_ref[...] - learn_rate * step_q
        new_o_ref[...] = wo_ref[...] - learn_rate * step_o

    p = p_ref[...]
    n = p.shape[0]
    pq = p[:, :64, :].reshape(n * 64, RANK)
    po = p[:, 64:, :].reshape(n * 32, RANK)
    uq = jnp.dot(pq, half_ref[:, :512], preferred_element_type=f32)
    uo = jnp.dot(po, half_ref[:, 512:1536], preferred_element_type=f32)
    wq = w_ref[:, :64, :].reshape(n * 64, 512)
    copy_q_ref[...] = (wq - learn_rate * (scale * uq)).astype(bf16)
    w0 = w_ref[:, 64:96, :].reshape(n * 32, 512)
    w1 = w_ref[:, 96:, :].reshape(n * 32, 512)
    copy_o_ref[:, :512] = (w0 - learn_rate * (scale * uo[:, :512])).astype(bf16)
    copy_o_ref[:, 512:] = (w1 - learn_rate * (scale * uo[:, 512:])).astype(bf16)


def finish(mine, other, half, rows, weight_query, weight_output, weights, factors):
    step = 8

    def whole(shape):
        return pl.BlockSpec(shape, lambda i: (0,) * len(shape))

    return pl.pallas_call(
        finish_kernel,
        grid=(FS // step,),
        in_specs=[
            SMEM,
            SMEM,
            whole((RANK, 1664)),
            whole((96, RANK)),
            whole((64, 512)),
            whole((32, 1024)),
            pl.BlockSpec((step, 128, 512), lambda i: (i, 0, 0)),
            pl.BlockSpec((step, 96, RANK), lambda i: (i, 0, 0)),
        ],
        out_specs=[
            pl.BlockSpec((step * 64, 512), lambda i: (i, 0)),
            pl.BlockSpec((step * 32, 1024), lambda i: (i, 0)),
            whole((64, 512)),
            whole((32, 1024)),
            whole((64, 512)),
            whole((32, 1024)),
        ],
        out_shape=[
            jax.ShapeDtypeStruct((D, 512), bf16),
            jax.ShapeDtypeStruct((DA, 1024), bf16),
            jax.ShapeDtypeStruct((64, 512), f32),
            jax.ShapeDtypeStruct((32, 1024), f32),
            jax.ShapeDtypeStruct((64, 512), f32),
            jax.ShapeDtypeStruct((32, 1024), f32),
        ],
        name="finish",
    )(mine, other, half, rows, weight_query, weight_output, weights, factors)


def local(
    inputs,
    query_cot,
    attended,
    output_cot,
    proj_query,
    proj_output,
    weight_query,
    weight_output,
    first_query,
    second_query,
    first_output,
    second_output,
):
    z, x = lax.axis_index("z"), lax.axis_index("x")
    rep, core = lax.axis_index("rep"), lax.axis_index("tp")
    fs = z * NX + x

    here = rep.reshape(1)

    weights = join(weight_query, weight_output)
    weights = lax.all_gather(weights, ("z", "x"), axis=0, tiled=True)

    cots = jnp.concatenate([query_cot, output_cot], axis=1)
    cots = [shifted(cots, "rep", 1), shifted(cots, "rep", 2), shifted(cots, "rep", 3)]

    piece = select(jnp.stack([rep, core]), proj_query, proj_output)
    piece = exchange(piece, "z")
    piece = from_everyone(piece.reshape(NZ * 24, 128), ("x", "rep"), 16)

    red, factors = project(piece, inputs, attended)
    red = red.reshape(8, 2, FS, 128)
    red = exchange(red, ("rep", "tp")).reshape(NREP, NTP, 2, FS, 128)
    part = exchange(partial_sums(here, red, [query_cot, output_cot] + cots), ("x", "z"))
    low, half = normed_payload(
        here, part, first_query, second_query, first_output, second_output
    )
    half = exchange(half, "z")
    low, half = lax.optimization_barrier((low, half))
    low_rows = [low, shifted(low, "rep", 1), shifted(low, "rep", 2), shifted(low, "rep", 3)]
    half = from_everyone(half.reshape(16, 1664), ("x", "rep"), 16).reshape(RANK, 1664)
    total = jnp.sum(half[:, 1536:].astype(f32)).reshape(1, 1)
    other = shifted(total, "tp", 1)

    others = shifted(factors, "tp", 1)
    k = lax.broadcasted_iota(jnp.int32, (128, RANK), 0)
    c = lax.broadcasted_iota(jnp.int32, (128, RANK), 1)
    spread = (c == 2 * k + core).astype(bf16)
    spread_other = (c == 2 * k + 1 - core).astype(bf16)
    whole = jnp.dot(factors.reshape(FS * 96, 128), spread, preferred_element_type=f32)
    whole = whole + jnp.dot(others.reshape(FS * 96, 128), spread_other, preferred_element_type=f32)
    whole = whole.astype(bf16).reshape(FS, 96, RANK)
    rows = lax.dynamic_index_in_dim(whole, fs, 0, keepdims=False)

    copy_q, copy_o, step_q, step_o, new_q, new_o = finish(
        total, other, half, rows, weight_query, weight_output,
        weights.reshape(FS, 128, 512), whole,
    )

    rolled = jnp.stack(low_rows)
    order = (rep - jnp.arange(NREP)) % NREP
    low_all = jnp.take(rolled, order, axis=0).reshape(8, 1536)
    first_q, second_q = moments(low_all[:, :512], first_query, second_query)
    first_o, second_o = moments(low_all[:, 512:], first_output, second_output)
    return (new_q, new_o, step_q, step_o, first_q, second_q, first_o, second_o, copy_q, copy_o)


def solution(mesh):
    devices = mesh.devices.reshape(NZ, NX, NREP, NTP)
    grid = Mesh(devices, ("z", "x", "rep", "tp"))
    fs = ("z", "x")
    tokens = ("z", "x", "rep")
    return jax.shard_map(
        local,
        mesh=grid,
        in_specs=(
            P(tokens, None),
            P(tokens, "tp"),
            P(tokens, None),
            P(tokens, "tp"),
            P(fs, None),
            P(fs, None),
            P(fs, "tp"),
            P(fs, "tp"),
            P(fs, "tp"),
            P(fs, "tp"),
            P(fs, "tp"),
            P(fs, "tp"),
        ),
        out_specs=(
            P(fs, "tp"),
            P(fs, "tp"),
            P(fs, "tp"),
            P(fs, "tp"),
            P(fs, "tp"),
            P(fs, "tp"),
            P(fs, "tp"),
            P(fs, "tp"),
            P(None, "tp"),
            P(None, "tp"),
        ),
        check_vma=False,
    )
```

```python
import jax
import jax.numpy as jnp
from jax import lax
from jax.experimental import pallas as pl
from jax.experimental.pallas import tpu as pltpu
from jax.sharding import Mesh, PartitionSpec as P


D = 2048
DA = 1024
RANK = 256
NZ, NX, NREP, NTP = 8, 4, 4, 2
FS = NZ * NX

beta_first = 0.9
beta_second = 0.95
adam_eps = 1e-08
mean_eps = 1e-06
learn_rate = 0.02

bf16 = jnp.bfloat16
f32 = jnp.float32


def exchange(pieces, axes):
    return lax.all_to_all(pieces, axes, split_axis=0, concat_axis=0, tiled=True)


def from_everyone(shard, axes, devices):
    return exchange(jnp.broadcast_to(shard, (devices, *shard.shape)), axes)


def shifted(array, axis, by):
    n = lax.axis_size(axis)
    return lax.ppermute(array, axis, [(i, (i + by) % n) for i in range(n)])


def one_hot(rows_of, columns, rows):
    r = lax.broadcasted_iota(jnp.int32, (rows, columns), 0)
    return (r == rows_of).astype(bf16)


def rank_of(core):
    k = lax.broadcasted_iota(jnp.int32, (1, RANK // NTP), 1)
    x, j, z = k // 32, (k // 8) % 4, k % 8
    return 8 * (4 * z + x) + 2 * j + core


VMEM = pl.BlockSpec(memory_space=pltpu.VMEM)


def near(array):
    return pltpu.with_memory_space_constraint(array, pltpu.VMEM)


SMEM = pl.BlockSpec(memory_space=pltpu.SMEM)


def coded(w):
    s = jnp.abs(w) * 2.0**18
    s = s * s
    s = s * s
    s = s * s
    return jnp.where(w < 0, -s, s).astype(bf16)


def decoded(code):
    v = code.astype(f32)
    s = jnp.abs(v)
    s = jnp.maximum(s, 2.0**-126)
    s = lax.rsqrt(lax.rsqrt(s * lax.rsqrt(s)))
    s = jnp.where(v == 0, 0.0, s * 2.0**-18)
    return jnp.where(v < 0, -s, s)


def join_kernel(query_ref, output_ref, both_ref):
    both_ref[:64] = coded(query_ref[...])
    both_ref[64:96] = coded(output_ref[:, :512])
    both_ref[96:] = coded(output_ref[:, 512:])


def join(query, output):
    return pl.pallas_call(
        join_kernel,
        in_specs=[VMEM, VMEM],
        out_specs=VMEM,
        out_shape=jax.ShapeDtypeStruct((128, 512), bf16),
        name="join",
    )(query, output)


def decode_kernel(code_ref, out_ref):
    out_ref[...] = decoded(code_ref[...])


def decode(codes):
    step = 8
    return pl.pallas_call(
        decode_kernel,
        grid=(FS // step,),
        in_specs=[pl.BlockSpec((step, 128, 512), lambda i: (i, 0, 0))],
        out_specs=pl.BlockSpec((step, 128, 512), lambda i: (i, 0, 0)),
        out_shape=jax.ShapeDtypeStruct((FS, 128, 512), f32),
        name="decode",
    )(pltpu.with_memory_space_constraint(codes, pltpu.HBM))


def project_kernel(factor_ref, inputs_ref, attended_ref, out_ref):
    factors_q = factor_ref[:, :64, :].reshape(D, 128)
    factors_o = factor_ref[:, 64:, :].reshape(DA, 128)
    for n, (left, right) in enumerate(((inputs_ref, factors_q), (attended_ref, factors_o))):
        red = jnp.dot(left[...], right, preferred_element_type=f32).T
        red = red.reshape(NX, NREP, NZ, 128)
        for j in range(NREP):
            mine = red[:, j].reshape(FS, 128)
            out_ref[j, 0, n] = mine
            out_ref[j, 1, n] = mine


def project(factors, inputs, attended):
    return pl.pallas_call(
        project_kernel,
        in_specs=[VMEM, VMEM, VMEM],
        out_specs=VMEM,
        out_shape=pltpu.VMEM((NREP, NTP, 2, FS, 128), f32),
        name="project",
    )(near(factors), near(inputs), near(attended))


def partial_kernel(rep_ref, red_ref, query_ref, output_ref, c1_ref, c2_ref, c3_ref, out_ref):
    rep = rep_ref[0]
    totals = [None, None]
    own = (query_ref[...], output_ref[...])
    sent = [(c[:, :512], c[:, 512:]) for c in (c1_ref, c2_ref, c3_ref)]
    for k, cots in enumerate([own] + sent):
        red = red_ref[lax.rem(rep + (NREP - k), NREP)]
        for n in range(2):
            left = red[:, n].reshape(64, 128)
            first = left.astype(bf16)
            rest = left - first.astype(f32)
            second = rest.astype(bf16)
            third = (rest - second.astype(f32)).astype(bf16)
            terms = jnp.concatenate([first, second, third], axis=0)
            part = jnp.dot(terms, cots[n], preferred_element_type=f32)
            totals[n] = part if totals[n] is None else totals[n] + part
    for n, (low, high) in enumerate(((0, 512), (512, 1536))):
        part = totals[n]
        part = part[:64] + (part[64:128] + part[128:])
        out_ref[:, 0, low:high] = part[:32]
        out_ref[:, 1, low:high] = part[32:]


def partial_sums(rep, red, cots):
    return pl.pallas_call(
        partial_kernel,
        in_specs=[SMEM] + [VMEM] * 6,
        out_specs=VMEM,
        out_shape=pltpu.VMEM((FS, NTP, 1536), f32),
        name="partial_sums",
    )(rep, near(red), *cots)


def moments(low_sum, first, second):
    first_new = beta_first * first + (1.0 - beta_first) * low_sum
    second_new = beta_second * second + (1.0 - beta_second) * low_sum * low_sum
    return first_new, second_new


def own_rows(ref, rep):
    value = ref[...]
    rows = value[:2]
    for k in range(1, NREP):
        rows = jnp.where(rep == k, value[2 * k : 2 * k + 2], rows)
    return rows


def normed_kernel(rep_ref, part_ref, fq_ref, sq_ref, fo_ref, so_ref, low_ref, half_ref):
    rep = rep_ref[0]
    low = part_ref[0]
    for k in range(1, FS):
        low = low + part_ref[k]
    low_ref[...] = low
    pieces = []
    total = jnp.zeros((2, 1), f32)
    for low_sum, first_ref, second_ref in (
        (low[:, :512], fq_ref, sq_ref),
        (low[:, 512:], fo_ref, so_ref),
    ):
        first_new, second_new = moments(low_sum, own_rows(first_ref, rep), own_rows(second_ref, rep))
        normed = first_new / (jnp.sqrt(second_new) + adam_eps)
        total = total + jnp.sum(normed * normed, axis=1, keepdims=True)
        pieces.append(normed.astype(bf16))
    high = total.astype(bf16).astype(f32)
    middle = (total - high).astype(bf16).astype(f32)
    last = total - high - middle
    lane = lax.broadcasted_iota(jnp.int32, (2, 128), 1)
    sums = jnp.where(lane == 0, high, jnp.where(lane == 1, middle, jnp.where(lane == 2, last, 0.0)))
    payload = jnp.concatenate(pieces + [sums.astype(bf16)], axis=1)
    for k in range(NZ):
        half_ref[k] = payload


def normed_payload(rep, part, first_query, second_query, first_output, second_output):
    return pl.pallas_call(
        normed_kernel,
        in_specs=[SMEM] + [VMEM] * 5,
        out_specs=[VMEM, VMEM],
        out_shape=[
            pltpu.VMEM((2, 1536), f32),
            pltpu.VMEM((NZ, 2, 1664), bf16),
        ],
        name="normed_payload",
    )(rep, *[near(a) for a in (part, first_query, second_query, first_output, second_output)])


CHUNKS = 4


def finish_kernel(
    mine_ref, other_ref, half_ref, rows_ref, wq_ref, wo_ref, p_ref, w_ref,
    copy_q_ref, copy_o_ref, step_q_ref, step_o_ref, new_q_ref, new_o_ref,
    w_buf, q_buf, o_buf, sq_buf, so_buf, nq_buf, no_buf, in_sem, out_sem,
):
    n = FS // CHUNKS
    arrivals = []
    for c in range(CHUNKS):
        part = pl.ds(c * n, n)
        arrivals.append(pltpu.make_async_copy(w_ref.at[part], w_buf.at[part], in_sem.at[c]))
        arrivals[-1].start()
    departures = []

    def send(source, target):
        departures.append(
            pltpu.make_async_copy(source, target, out_sem.at[len(departures)])
        )
        departures[-1].start()

    total = jnp.full((1, 128), mine_ref[0, 0] + other_ref[0, 0], f32)
    scale = lax.rsqrt(total / (RANK * (DA + D)) + mean_eps)[:, :1]

    rows = rows_ref[...]
    step_q = scale * jnp.dot(rows[:64], half_ref[:, :512], preferred_element_type=f32)
    step_o = scale * jnp.dot(rows[64:], half_ref[:, 512:1536], preferred_element_type=f32)
    sq_buf[...] = step_q
    so_buf[...] = step_o
    nq_buf[...] = wq_ref[...] - learn_rate * step_q
    no_buf[...] = wo_ref[...] - learn_rate * step_o
    send(sq_buf, step_q_ref)
    send(so_buf, step_o_ref)
    send(nq_buf, new_q_ref)
    send(no_buf, new_o_ref)

    for c in range(CHUNKS):
        part = pl.ds(c * n, n)
        pq = p_ref[part, :64, :].reshape(n * 64, RANK)
        po = p_ref[part, 64:, :].reshape(n * 32, RANK)
        uq = jnp.dot(pq, half_ref[:, :512], preferred_element_type=f32)
        uo = jnp.dot(po, half_ref[:, 512:1536], preferred_element_type=f32)
        arrivals[c].wait()
        q_rows, o_rows = pl.ds(c * n * 64, n * 64), pl.ds(c * n * 32, n * 32)
        wq = w_buf[part, :64, :].reshape(n * 64, 512)
        q_buf[q_rows, :] = (wq - learn_rate * (scale * uq)).astype(bf16)
        w0 = w_buf[part, 64:96, :].reshape(n * 32, 512)
        w1 = w_buf[part, 96:, :].reshape(n * 32, 512)
        o_buf[o_rows, :512] = (w0 - learn_rate * (scale * uo[:, :512])).astype(bf16)
        o_buf[o_rows, 512:] = (w1 - learn_rate * (scale * uo[:, 512:])).astype(bf16)
        send(q_buf.at[q_rows], copy_q_ref.at[q_rows])
        send(o_buf.at[o_rows], copy_o_ref.at[o_rows])
    for departure in departures:
        departure.wait()


def finish(mine, other, half, rows, weight_query, weight_output, weights, factors):
    hbm = pl.BlockSpec(memory_space=pl.ANY)
    leaving = [
        jax.ShapeDtypeStruct((D, 512), bf16),
        jax.ShapeDtypeStruct((DA, 1024), bf16),
        jax.ShapeDtypeStruct((64, 512), f32),
        jax.ShapeDtypeStruct((32, 1024), f32),
        jax.ShapeDtypeStruct((64, 512), f32),
        jax.ShapeDtypeStruct((32, 1024), f32),
    ]
    return pl.pallas_call(
        finish_kernel,
        in_specs=[SMEM, SMEM] + [VMEM] * 5 + [hbm],
        out_specs=[hbm] * 6,
        out_shape=leaving,
        scratch_shapes=[pltpu.VMEM((FS, 128, 512), f32)]
        + [pltpu.VMEM(a.shape, a.dtype) for a in leaving]
        + [pltpu.SemaphoreType.DMA((CHUNKS,)), pltpu.SemaphoreType.DMA((4 + 2 * CHUNKS,))],
        compiler_params=pltpu.CompilerParams(vmem_limit_bytes=32 * 2**20),
        name="finish",
    )(
        mine,
        other,
        *[near(a) for a in (half, rows, weight_query, weight_output, factors)],
        pltpu.with_memory_space_constraint(weights, pltpu.HBM),
    )


def local(
    inputs,
    query_cot,
    attended,
    output_cot,
    proj_query,
    proj_output,
    weight_query,
    weight_output,
    first_query,
    second_query,
    first_output,
    second_output,
):
    z, x = lax.axis_index("z"), lax.axis_index("x")
    rep, core = lax.axis_index("rep"), lax.axis_index("tp")
    fs = z * NX + x

    here = rep.reshape(1)

    weights = join(weight_query, weight_output)
    weights = lax.all_gather(weights, ("z", "x"), axis=0, tiled=True)
    weights = decode(weights.reshape(FS, 128, 512))

    cots = jnp.concatenate([query_cot, output_cot], axis=1)
    cots = [shifted(cots, "rep", 1), shifted(cots, "rep", 2), shifted(cots, "rep", 3)]

    both = jnp.concatenate([proj_query, proj_output], axis=0)
    mine = jnp.dot(both, one_hot(rank_of(core), 128, RANK), preferred_element_type=f32)
    factors = from_everyone(mine.astype(bf16).reshape(96, 128), ("z", "x"), FS)

    red = project(factors, inputs, attended).reshape(8, 2, FS, 128)
    red = exchange(red, ("rep", "tp")).reshape(NREP, NTP, 2, FS, 128)
    part = partial_sums(here, red, [query_cot, output_cot] + cots)
    part = exchange(part, ("x", "z"))
    low, half = normed_payload(
        here, part, first_query, second_query, first_output, second_output
    )
    half = exchange(half, "z")
    low_rows = [low, shifted(low, "rep", 1), shifted(low, "rep", 2), shifted(low, "rep", 3)]
    half = from_everyone(half.reshape(16, 1664), ("x", "rep"), 16).reshape(RANK, 1664)
    total = jnp.sum(half[:, 1536:].astype(f32)).reshape(1, 1)
    other = shifted(total, "tp", 1)

    others = shifted(factors, "tp", 1)
    k = lax.broadcasted_iota(jnp.int32, (128, RANK), 0)
    c = lax.broadcasted_iota(jnp.int32, (128, RANK), 1)
    spread = (c == 2 * k + core).astype(bf16)
    spread_other = (c == 2 * k + 1 - core).astype(bf16)
    whole = jnp.dot(factors.reshape(FS * 96, 128), spread, preferred_element_type=f32)
    whole = whole + jnp.dot(others.reshape(FS * 96, 128), spread_other, preferred_element_type=f32)
    whole = whole.astype(bf16).reshape(FS, 96, RANK)
    rows = lax.dynamic_index_in_dim(whole, fs, 0, keepdims=False)

    copy_q, copy_o, step_q, step_o, new_q, new_o = finish(
        total, other, half, rows, weight_query, weight_output,
        weights, whole,
    )

    rolled = jnp.stack(low_rows)
    order = (rep - jnp.arange(NREP)) % NREP
    low_all = jnp.take(rolled, order, axis=0).reshape(8, 1536)
    first_q, second_q = moments(low_all[:, :512], first_query, second_query)
    first_o, second_o = moments(low_all[:, 512:], first_output, second_output)
    return (new_q, new_o, step_q, step_o, first_q, second_q, first_o, second_o, copy_q, copy_o)


def solution(mesh):
    devices = mesh.devices.reshape(NZ, NX, NREP, NTP)
    grid = Mesh(devices, ("z", "x", "rep", "tp"))
    fs = ("z", "x")
    tokens = ("z", "x", "rep")
    return jax.shard_map(
        local,
        mesh=grid,
        in_specs=(
            P(tokens, None),
            P(tokens, "tp"),
            P(tokens, None),
            P(tokens, "tp"),
            P(fs, None),
            P(fs, None),
            P(fs, "tp"),
            P(fs, "tp"),
            P(fs, "tp"),
            P(fs, "tp"),
            P(fs, "tp"),
            P(fs, "tp"),
        ),
        out_specs=(
            P(fs, "tp"),
            P(fs, "tp"),
            P(fs, "tp"),
            P(fs, "tp"),
            P(fs, "tp"),
            P(fs, "tp"),
            P(fs, "tp"),
            P(fs, "tp"),
            P(None, "tp"),
            P(None, "tp"),
        ),
        check_vma=False,
    )
```

```python
import jax
import jax.numpy as jnp
from jax import lax
from jax.experimental import pallas as pl
from jax.experimental.pallas import tpu as pltpu
from jax.sharding import Mesh, PartitionSpec as P


D = 2048
DA = 1024
RANK = 256
NZ, NX, NREP, NTP = 8, 4, 4, 2
FS = NZ * NX

beta_first = 0.9
beta_second = 0.95
adam_eps = 1e-08
mean_eps = 1e-06
learn_rate = 0.02

bf16 = jnp.bfloat16
f32 = jnp.float32


def exchange(pieces, axes):
    return lax.all_to_all(pieces, axes, split_axis=0, concat_axis=0, tiled=True)


def from_everyone(shard, axes, devices):
    return exchange(jnp.broadcast_to(shard, (devices, *shard.shape)), axes)


def shifted(array, axis, by):
    n = lax.axis_size(axis)
    return lax.ppermute(array, axis, [(i, (i + by) % n) for i in range(n)])


VMEM = pl.BlockSpec(memory_space=pltpu.VMEM)


def near(array):
    return pltpu.with_memory_space_constraint(array, pltpu.VMEM)


SMEM = pl.BlockSpec(memory_space=pltpu.SMEM)


def coded(w):
    s = jnp.abs(w) * 2.0**18
    s = s * s
    s = s * s
    s = s * s
    return jnp.where(w < 0, -s, s).astype(bf16)


def decoded(code):
    v = code.astype(f32)
    s = jnp.abs(v)
    s = jnp.maximum(s, 2.0**-126)
    s = lax.rsqrt(lax.rsqrt(s * lax.rsqrt(s)))
    s = jnp.where(v == 0, 0.0, s * 2.0**-18)
    return jnp.where(v < 0, -s, s)


def prepare_kernel(core_ref, wq_ref, wo_ref, pq_ref, po_ref, code_ref, factor_ref):
    k = lax.broadcasted_iota(jnp.int32, (RANK, 128), 1)
    r = lax.broadcasted_iota(jnp.int32, (RANK, 128), 0)
    core = core_ref[0]
    ranks = (r == 32 * (k % 8) + 8 * (k // 32) + 2 * ((k // 8) % 4) + core).astype(bf16)
    both = jnp.concatenate([pq_ref[...], po_ref[...]], axis=0)
    mine = jnp.dot(both, ranks, preferred_element_type=f32).astype(bf16)
    for n in range(FS):
        factor_ref[n] = mine
    code_ref[:64] = coded(wq_ref[...])
    code_ref[64:96] = coded(wo_ref[:, :512])
    code_ref[96:] = coded(wo_ref[:, 512:])


def prepare(core, weight_query, weight_output, proj_query, proj_output):
    return pl.pallas_call(
        prepare_kernel,
        in_specs=[SMEM] + [VMEM] * 4,
        out_specs=[VMEM, VMEM],
        out_shape=[
            jax.ShapeDtypeStruct((128, 512), bf16),
            jax.ShapeDtypeStruct((FS, 96, 128), bf16),
        ],
        name="prepare",
    )(core, weight_query, weight_output, proj_query, proj_output)


def decode_kernel(code_ref, out_ref):
    out_ref[...] = decoded(code_ref[...])


def decode(codes):
    step = 8
    return pl.pallas_call(
        decode_kernel,
        grid=(FS // step,),
        in_specs=[pl.BlockSpec((step, 128, 512), lambda i: (i, 0, 0))],
        out_specs=pl.BlockSpec((step, 128, 512), lambda i: (i, 0, 0)),
        out_shape=jax.ShapeDtypeStruct((FS, 128, 512), f32),
        name="decode",
    )(pltpu.with_memory_space_constraint(codes, pltpu.HBM))


def project_kernel(factor_ref, inputs_ref, attended_ref, out_ref):
    factors_q = factor_ref[:, :64, :].reshape(D, 128)
    factors_o = factor_ref[:, 64:, :].reshape(DA, 128)
    for n, (left, right) in enumerate(((inputs_ref, factors_q), (attended_ref, factors_o))):
        red = jnp.dot(left[...], right, preferred_element_type=f32).T
        red = red.reshape(NX, NREP, NZ, 128)
        for j in range(NREP):
            mine = red[:, j].reshape(FS, 128)
            out_ref[j, 0, n] = mine
            out_ref[j, 1, n] = mine


def project(factors, inputs, attended):
    return pl.pallas_call(
        project_kernel,
        in_specs=[VMEM, VMEM, VMEM],
        out_specs=VMEM,
        out_shape=pltpu.VMEM((NREP, NTP, 2, FS, 128), f32),
        name="project",
    )(near(factors), near(inputs), near(attended))


def partial_kernel(rep_ref, red_ref, query_ref, output_ref, c1_ref, c2_ref, c3_ref, out_ref):
    rep = rep_ref[0]
    totals = [None, None]
    own = (query_ref[...], output_ref[...])
    sent = [(c[:, :512], c[:, 512:]) for c in (c1_ref, c2_ref, c3_ref)]
    for k, cots in enumerate([own] + sent):
        red = red_ref[lax.rem(rep + (NREP - k), NREP)]
        for n in range(2):
            left = red[:, n].reshape(64, 128)
            first = left.astype(bf16)
            rest = left - first.astype(f32)
            second = rest.astype(bf16)
            third = (rest - second.astype(f32)).astype(bf16)
            terms = jnp.concatenate([first, second, third], axis=0)
            part = jnp.dot(terms, cots[n], preferred_element_type=f32)
            totals[n] = part if totals[n] is None else totals[n] + part
    for n, (low, high) in enumerate(((0, 512), (512, 1536))):
        part = totals[n]
        part = part[:64] + (part[64:128] + part[128:])
        out_ref[:, 0, low:high] = part[:32]
        out_ref[:, 1, low:high] = part[32:]


def partial_sums(rep, red, cots):
    return pl.pallas_call(
        partial_kernel,
        in_specs=[SMEM] + [VMEM] * 6,
        out_specs=VMEM,
        out_shape=pltpu.VMEM((FS, NTP, 1536), f32),
        compiler_params=pltpu.CompilerParams(vmem_limit_bytes=16 * 2**20),
        name="partial_sums",
    )(rep, near(red), *cots)


def moments(low_sum, first, second):
    first_new = beta_first * first + (1.0 - beta_first) * low_sum
    second_new = beta_second * second + (1.0 - beta_second) * low_sum * low_sum
    return first_new, second_new


def own_rows(ref, rep):
    value = ref[...]
    rows = value[:2]
    for k in range(1, NREP):
        rows = jnp.where(rep == k, value[2 * k : 2 * k + 2], rows)
    return rows


def normed_kernel(rep_ref, part_ref, fq_ref, sq_ref, fo_ref, so_ref, low_ref, half_ref):
    rep = rep_ref[0]
    low = part_ref[0]
    for k in range(1, FS):
        low = low + part_ref[k]
    low_ref[...] = low
    pieces = []
    total = jnp.zeros((2, 1), f32)
    for low_sum, first_ref, second_ref in (
        (low[:, :512], fq_ref, sq_ref),
        (low[:, 512:], fo_ref, so_ref),
    ):
        first_new, second_new = moments(low_sum, own_rows(first_ref, rep), own_rows(second_ref, rep))
        normed = first_new / (jnp.sqrt(second_new) + adam_eps)
        total = total + jnp.sum(normed * normed, axis=1, keepdims=True)
        pieces.append(normed.astype(bf16))
    high = total.astype(bf16).astype(f32)
    middle = (total - high).astype(bf16).astype(f32)
    last = total - high - middle
    lane = lax.broadcasted_iota(jnp.int32, (2, 128), 1)
    sums = jnp.where(lane == 0, high, jnp.where(lane == 1, middle, jnp.where(lane == 2, last, 0.0)))
    payload = jnp.concatenate(pieces + [sums.astype(bf16)], axis=1)
    for k in range(NZ):
        half_ref[k] = payload


def normed_payload(rep, part, first_query, second_query, first_output, second_output):
    return pl.pallas_call(
        normed_kernel,
        in_specs=[SMEM] + [VMEM] * 5,
        out_specs=[VMEM, VMEM],
        out_shape=[
            pltpu.VMEM((2, 1536), f32),
            pltpu.VMEM((NZ, 2, 1664), bf16),
        ],
        compiler_params=pltpu.CompilerParams(vmem_limit_bytes=16 * 2**20),
        name="normed_payload",
    )(rep, *[near(a) for a in (part, first_query, second_query, first_output, second_output)])


CHUNKS = 4


def finish_kernel(
    mine_ref, other_ref, half_ref, rows_ref, wq_ref, wo_ref, p_ref, w_ref,
    copy_q_ref, copy_o_ref, step_q_ref, step_o_ref, new_q_ref, new_o_ref,
    w_buf, q_buf, o_buf, sq_buf, so_buf, nq_buf, no_buf, in_sem, out_sem,
):
    n = FS // CHUNKS
    arrivals = []
    for c in range(CHUNKS):
        part = pl.ds(c * n, n)
        arrivals.append(pltpu.make_async_copy(w_ref.at[part], w_buf.at[part], in_sem.at[c]))
        arrivals[-1].start()
    departures = []

    def send(source, target):
        departures.append(
            pltpu.make_async_copy(source, target, out_sem.at[len(departures)])
        )
        departures[-1].start()

    total = jnp.full((1, 128), mine_ref[0, 0] + other_ref[0, 0], f32)
    scale = lax.rsqrt(total / (RANK * (DA + D)) + mean_eps)[:, :1]

    rows = rows_ref[...]
    step_q = scale * jnp.dot(rows[:64], half_ref[:, :512], preferred_element_type=f32)
    step_o = scale * jnp.dot(rows[64:], half_ref[:, 512:1536], preferred_element_type=f32)
    sq_buf[...] = step_q
    so_buf[...] = step_o
    nq_buf[...] = wq_ref[...] - learn_rate * step_q
    no_buf[...] = wo_ref[...] - learn_rate * step_o
    send(sq_buf, step_q_ref)
    send(so_buf, step_o_ref)
    send(nq_buf, new_q_ref)
    send(no_buf, new_o_ref)

    for c in range(CHUNKS):
        part = pl.ds(c * n, n)
        pq = p_ref[part, :64, :].reshape(n * 64, RANK)
        po = p_ref[part, 64:, :].reshape(n * 32, RANK)
        uq = jnp.dot(pq, half_ref[:, :512], preferred_element_type=f32)
        uo = jnp.dot(po, half_ref[:, 512:1536], preferred_element_type=f32)
        arrivals[c].wait()
        q_rows, o_rows = pl.ds(c * n * 64, n * 64), pl.ds(c * n * 32, n * 32)
        wq = w_buf[part, :64, :].reshape(n * 64, 512)
        q_buf[q_rows, :] = (wq - learn_rate * (scale * uq)).astype(bf16)
        w0 = w_buf[part, 64:96, :].reshape(n * 32, 512)
        w1 = w_buf[part, 96:, :].reshape(n * 32, 512)
        o_buf[o_rows, :512] = (w0 - learn_rate * (scale * uo[:, :512])).astype(bf16)
        o_buf[o_rows, 512:] = (w1 - learn_rate * (scale * uo[:, 512:])).astype(bf16)
        send(q_buf.at[q_rows], copy_q_ref.at[q_rows])
        send(o_buf.at[o_rows], copy_o_ref.at[o_rows])
    for departure in departures:
        departure.wait()


def finish(mine, other, half, rows, weight_query, weight_output, weights, factors):
    hbm = pl.BlockSpec(memory_space=pl.ANY)
    leaving = [
        jax.ShapeDtypeStruct((D, 512), bf16),
        jax.ShapeDtypeStruct((DA, 1024), bf16),
        jax.ShapeDtypeStruct((64, 512), f32),
        jax.ShapeDtypeStruct((32, 1024), f32),
        jax.ShapeDtypeStruct((64, 512), f32),
        jax.ShapeDtypeStruct((32, 1024), f32),
    ]
    return pl.pallas_call(
        finish_kernel,
        in_specs=[SMEM, SMEM] + [VMEM] * 5 + [hbm],
        out_specs=[hbm] * 6,
        out_shape=leaving,
        scratch_shapes=[pltpu.VMEM((FS, 128, 512), f32)]
        + [pltpu.VMEM(a.shape, a.dtype) for a in leaving]
        + [pltpu.SemaphoreType.DMA((CHUNKS,)), pltpu.SemaphoreType.DMA((4 + 2 * CHUNKS,))],
        compiler_params=pltpu.CompilerParams(vmem_limit_bytes=32 * 2**20),
        name="finish",
    )(
        mine,
        other,
        *[near(a) for a in (half, rows, weight_query, weight_output, factors)],
        pltpu.with_memory_space_constraint(weights, pltpu.HBM),
    )


def local(
    inputs,
    query_cot,
    attended,
    output_cot,
    proj_query,
    proj_output,
    weight_query,
    weight_output,
    first_query,
    second_query,
    first_output,
    second_output,
):
    z, x = lax.axis_index("z"), lax.axis_index("x")
    rep, core = lax.axis_index("rep"), lax.axis_index("tp")
    fs = z * NX + x

    here = rep.reshape(1)

    weights, factors = prepare(
        core.reshape(1), weight_query, weight_output, proj_query, proj_output
    )
    weights = lax.all_gather(weights, ("z", "x"), axis=0, tiled=True)
    weights = decode(weights.reshape(FS, 128, 512))

    cots = jnp.concatenate([query_cot, output_cot], axis=1)
    cots = [shifted(cots, "rep", 1), shifted(cots, "rep", 2), shifted(cots, "rep", 3)]

    factors = exchange(factors, ("z", "x"))

    red = project(factors, inputs, attended).reshape(8, 2, FS, 128)
    red = exchange(red, ("rep", "tp")).reshape(NREP, NTP, 2, FS, 128)
    part = partial_sums(here, red, [query_cot, output_cot] + cots)
    part = exchange(part, ("x", "z"))
    low, half = normed_payload(
        here, part, first_query, second_query, first_output, second_output
    )
    half = exchange(half, "z")
    low_rows = [low, shifted(low, "rep", 1), shifted(low, "rep", 2), shifted(low, "rep", 3)]
    half = from_everyone(half.reshape(16, 1664), ("x", "rep"), 16).reshape(RANK, 1664)
    total = jnp.sum(half[:, 1536:].astype(f32)).reshape(1, 1)
    other = shifted(total, "tp", 1)

    others = shifted(factors, "tp", 1)
    k = lax.broadcasted_iota(jnp.int32, (128, RANK), 0)
    c = lax.broadcasted_iota(jnp.int32, (128, RANK), 1)
    spread = (c == 2 * k + core).astype(bf16)
    spread_other = (c == 2 * k + 1 - core).astype(bf16)
    whole = jnp.dot(factors.reshape(FS * 96, 128), spread, preferred_element_type=f32)
    whole = whole + jnp.dot(others.reshape(FS * 96, 128), spread_other, preferred_element_type=f32)
    whole = whole.astype(bf16).reshape(FS, 96, RANK)
    rows = lax.dynamic_index_in_dim(whole, fs, 0, keepdims=False)

    copy_q, copy_o, step_q, step_o, new_q, new_o = finish(
        total, other, half, rows, weight_query, weight_output,
        weights, whole,
    )

    rolled = jnp.stack(low_rows)
    order = (rep - jnp.arange(NREP)) % NREP
    low_all = jnp.take(rolled, order, axis=0).reshape(8, 1536)
    first_q, second_q = moments(low_all[:, :512], first_query, second_query)
    first_o, second_o = moments(low_all[:, 512:], first_output, second_output)
    return (new_q, new_o, step_q, step_o, first_q, second_q, first_o, second_o, copy_q, copy_o)


def solution(mesh):
    devices = mesh.devices.reshape(NZ, NX, NREP, NTP)
    grid = Mesh(devices, ("z", "x", "rep", "tp"))
    fs = ("z", "x")
    tokens = ("z", "x", "rep")
    return jax.shard_map(
        local,
        mesh=grid,
        in_specs=(
            P(tokens, None),
            P(tokens, "tp"),
            P(tokens, None),
            P(tokens, "tp"),
            P(fs, None),
            P(fs, None),
            P(fs, "tp"),
            P(fs, "tp"),
            P(fs, "tp"),
            P(fs, "tp"),
            P(fs, "tp"),
            P(fs, "tp"),
        ),
        out_specs=(
            P(fs, "tp"),
            P(fs, "tp"),
            P(fs, "tp"),
            P(fs, "tp"),
            P(fs, "tp"),
            P(fs, "tp"),
            P(fs, "tp"),
            P(fs, "tp"),
            P(None, "tp"),
            P(None, "tp"),
        ),
        check_vma=False,
    )
```
